512 devices in a mesh: gr: 2 (over z_hi), fs: 32 (over z_lo, y), tp: 8 (over x, core).
Axes of the slice: x: 4, y: 8, z: 8 (z_hi: 2, z_lo: 4; z = z_hi * 4 + z_lo), core: 2. Of those that a mesh axis runs over, the one named last changes fastest.
Arguments:
- prompt: bfloat16 [8192, 2048], P(('gr', 'fs')), may hold values from -6 to 6
- expert_ids: int32 [8192, 2], P(('gr', 'fs')), may hold values from 0 to 7, all different within a row; in each aligned block of 128 rows (0 to 127, 128 to 255, ...) at most 32 rows name the same one
- route_weights: float32 [8192, 2], P(('gr', 'fs')), may hold values from 0.2 to 1
- gate_master: float32 [8, 2048, 8192], P('gr', 'fs', 'tp'), may hold values from -0.125 to 0.125
- up_master: float32 [8, 2048, 8192], P('gr', 'fs', 'tp'), may hold values from -0.125 to 0.125
- down_master: float32 [8, 8192, 2048], P('gr', 'fs', 'tp'), may hold values from -0.0625 to 0.0625
- ffn_gain: float32 [2048], P('fs'), may hold values from 0.1 to 1.9
Outputs:
- gate_serving: bfloat16 [8, 2048, 8192], P('tp', None, 'fs')
- up_serving: bfloat16 [8, 2048, 8192], P('tp', None, 'fs')
- down_serving: bfloat16 [8, 8192, 2048], P('tp', 'fs')
- mixed: bfloat16 [8192, 2048], P(('gr', 'fs', 'tp'))
The draws below stay inside these ranges and needn't reach their ends.
Inputs may be any that keep to these rules, and one draw needn't show every extreme that they name: `expert_ids`: the two experts of a token differ; the rows of one index of gr and fs name each expert exactly 32 times.
All inputs are finite; a program needn't handle non-finite values.
Results may differ from the reference program's by a relative error of at most 0.025.
Values may be sent and summed in bfloat16 or wider, within the bound.
A program may use at most 64 MiB of HBM per device.

```python
import math
import jax
import jax.numpy as jnp
import numpy as np
from jax import lax

D = 2048
FF = 8192
EXPERTS = 8
TOK_DEV = 128
SLOTS = 32
TOKENS = 8192
N_FS = 32


def block_scale(own_key, dims, cuts, low, largest):
    gain, own = 1.0, jax.random.fold_in(own_key, 6)
    for axis_at, parts in cuts:
        steps = jnp.exp(jax.random.uniform(jax.random.fold_in(own, axis_at), (parts,), jnp.float32, low / len(cuts), largest / len(cuts)))
        gain = gain * jnp.repeat(steps, dims[axis_at] // parts).reshape([-1 if axis == axis_at else 1 for axis in range(len(dims))])
    return gain


def deal_out(stream_key, own, number, rows, amount, top, reach, slope):
    sequence = jax.random.permutation(stream_key, amount)
    heavy_load, ordinary = load_shares(amount, rows * top, reach, slope, True), load_shares(amount, rows * top, reach, slope, False)
    places = jnp.arange(amount)

    def named(tallies, offset_by):
        used = int((tallies > 0).sum())
        fixed = max(1, used // 4)
        shifted = fixed + (places - fixed + offset_by * (used - fixed)) % max(1, amount - fixed)
        return jnp.zeros((amount,), jnp.int32).at[sequence[jnp.where(places < fixed, places, shifted)]].set(jnp.asarray(tallies, jnp.int32))

    tallies = jnp.where(number % 4 == 0, named(heavy_load, number // 4), named(ordinary, number - number // 4 - 1))
    mixed = jax.random.permutation(jax.random.fold_in(own, 3), amount)
    giver, sink = mixed[0:amount // 2 * 2:2], mixed[1:amount // 2 * 2:2]
    margin = jnp.minimum(tallies[giver] - 1, reach - tallies[sink]) // 2
    margin = jnp.where((giver == sequence[0]) | (sink == sequence[0]) | (tallies[sink] == 0), 0, jnp.maximum(margin, 0))
    shifted = jax.random.randint(jax.random.fold_in(own, 4), (amount // 2,), 0, 1 << 20) % (margin + 1)
    tallies = tallies.at[giver].add(-shifted).at[sink].add(shifted)
    items = jnp.searchsorted(jnp.cumsum(tallies), jnp.arange(rows * top), side="right").astype(jnp.int32)
    grid = items.reshape(top, rows).T
    grid = grid[jax.random.permutation(jax.random.fold_in(own, 1), rows)]
    offset_by = jax.random.randint(jax.random.fold_in(own, 2), (rows, 1), 0, top)
    return jnp.take_along_axis(grid, (jnp.arange(top)[None, :] + offset_by) % top, axis=1)


def load_shares(amount, total, bound, skew, full):
    portions = [(1 << 20) // math.isqrt(grade ** skew) + 1 for grade in range(1, amount + 1)]
    largest = bound if full else min(bound, max(-(-total // amount), total * portions[0] // sum(portions)))
    least = 1 if total - largest >= amount - 1 else 0
    holding, spare = [largest] + [least] * (amount - 1), total - largest - least * (amount - 1)
    while spare > 0:
        free = [i for i in range(1, amount) if holding[i] < largest] or [i for i in range(1, amount) if holding[i] < bound]
        whole, left = sum([portions[i] for i in free]), spare
        for i in free:
            more = min(bound - holding[i], max(1, left * portions[i] // whole), spare)
            holding[i] = holding[i] + more
            spare = spare - more
    return np.array(holding)


def gaussian(stream_key, extent, scale, limit, pieces=(), kind=jnp.bfloat16):
    factor_of = block_scale(stream_key, extent, pieces, -0.22, 0.18) if pieces else 1.0
    drawn = jax.random.normal(stream_key, extent, jnp.float32) * scale * factor_of
    return jnp.minimum(jnp.maximum(drawn, -limit), limit).astype(kind)


def setup_inputs(seed: int = 0) -> dict:
    keys = jax.random.split(jax.random.key(seed), 8)
    prompt = gaussian(keys[0], (TOKENS, D), 1.0, 6.0, ((0, 64),))
    expert_ids_keys = jax.random.split(jax.random.fold_in(keys[1], 1), TOKENS // TOK_DEV)
    expert_ids_turns = jax.random.permutation(jax.random.fold_in(keys[1], 3), TOKENS // TOK_DEV)
    expert_ids = jax.vmap(lambda own, number: deal_out(jax.random.fold_in(keys[1], 2), own, number, TOK_DEV, EXPERTS, 2, SLOTS, 0))(expert_ids_keys, expert_ids_turns).reshape((TOKENS, 2))
    route_weights = jnp.clip(0.2 + 0.8 * jax.random.uniform(keys[2], (TOKENS, 2), jnp.float32) ** block_scale(keys[2], (TOKENS, 2), ((0, 64),), -0.2, 0.2), 0.2, 1.0)
    gate_master = gaussian(keys[3], (EXPERTS, D, FF), D ** -0.5, 0.125, ((0, 2), (1, 32), (2, 8)), jnp.float32)
    up_master = gaussian(keys[4], (EXPERTS, D, FF), D ** -0.5, 0.125, ((0, 2), (1, 32), (2, 8)), jnp.float32)
    down_master = gaussian(keys[5], (EXPERTS, FF, D), FF ** -0.5, 0.0625, ((0, 2), (1, 32), (2, 8)), jnp.float32)
    ffn_gain = jnp.clip(1.0 + 0.18 * jax.random.normal(keys[6], (D,), jnp.float32), 0.1, 1.9)
    return dict(prompt=prompt, expert_ids=expert_ids, route_weights=route_weights, gate_master=gate_master, up_master=up_master, down_master=down_master, ffn_gain=ffn_gain)


NORM_EPS = 1e-06

def reference(prompt, expert_ids, route_weights, gate_master, up_master, down_master, ffn_gain):
    folding = ffn_gain[None, :, None]
    gate_serving = (gate_master * folding).astype(jnp.bfloat16)
    up_serving = (up_master * folding).astype(jnp.bfloat16)
    down_serving = down_master.astype(jnp.bfloat16)
    xfloat = prompt.astype(jnp.float32)
    normed = (xfloat * lax.rsqrt(lax.optimization_barrier(jnp.mean(xfloat * xfloat, axis=1, keepdims=True)) + NORM_EPS)).astype(jnp.bfloat16)
    pair_expert = expert_ids.reshape(-1)
    pair_weight = route_weights.reshape(-1)
    chosen = TOKENS * 2 // EXPERTS
    slice_width = FF // N_FS
    terms = jnp.zeros((TOKENS * 2, D), jnp.bfloat16)
    for expert in range(EXPERTS):
        ordering = jnp.argsort((pair_expert != expert).astype(jnp.int32), stable=True)[:chosen].astype(jnp.int32)
        rows_in = normed[ordering // 2]
        gate_part = jnp.dot(rows_in, gate_serving[expert], preferred_element_type=jnp.float32)
        up_part = jnp.dot(rows_in, up_serving[expert], preferred_element_type=jnp.float32)
        hidden = (jax.nn.silu(gate_part) * up_part).astype(jnp.bfloat16)
        down_one = down_serving[expert]

        def add_slice(total, index):
            start_row = (index * slice_width).astype(jnp.int32)
            hidden_block = lax.dynamic_slice_in_dim(hidden, start_row, slice_width, 1)
            weights = lax.dynamic_slice_in_dim(down_one, start_row, slice_width, 0)
            partial_sum = lax.optimization_barrier(jnp.dot(hidden_block, weights, preferred_element_type=jnp.float32).astype(jnp.bfloat16))
            return (total + partial_sum.astype(jnp.float32), None)
        expert_out, _ = lax.scan(add_slice, jnp.zeros((chosen, D), jnp.float32), jnp.arange(N_FS, dtype=jnp.int32))
        terms = terms.at[ordering].set((expert_out * pair_weight[ordering][:, None]).astype(jnp.bfloat16))
    mixed = lax.optimization_barrier(jnp.sum(terms.reshape(TOKENS, 2, D).astype(jnp.float32), axis=1)).astype(jnp.bfloat16)
    return (gate_serving, up_serving, down_serving, mixed)
```

```python
import functools

import jax
import jax.numpy as jnp
from jax import lax
from jax.experimental import pallas as pl
from jax.experimental.pallas import tpu as pltpu
from jax.sharding import PartitionSpec as P

EXPERTS = 8
SLOTS = 32
TOK = 128
D = 2048
NORM_EPS = 1e-06
MESH = pl.DeviceIdType.MESH
BF = jnp.bfloat16
F32 = jnp.float32


def place():
    g, f, t = lax.axis_index("gr"), lax.axis_index("fs"), lax.axis_index("tp")
    return g, lax.div(f, 8), lax.rem(f, 8), lax.div(t, 2), lax.rem(t, 2)


def dev(g, zl, y, x, c):
    return (g, zl * 8 + y, x * 2 + c)


def signal(sem, where):
    pl.semaphore_signal(sem, inc=1, device_id=where, device_id_type=MESH)


def rcopy(src, dst, ssem, rsem, where):
    return pltpu.make_async_remote_copy(
        src_ref=src, dst_ref=dst, send_sem=ssem, recv_sem=rsem, device_id=where, device_id_type=MESH
    )


def arrived(buf, sem):
    pltpu.make_async_copy(buf, buf, sem).wait()


def home_of(g, el):
    odd = lax.rem(el, 2)
    x1 = 2 * g + lax.div(el, 2)
    return x1, odd, x1 * (1 - odd) + (3 - x1) * odd


def served_by(g, x):
    h = lax.div(x, 2)
    c1 = h + g - 2 * h * g
    return x * (1 - c1) + (3 - x) * c1, c1


def choice_matrix(ids):
    e = lax.axis_index("tp")
    hit = (ids == e).astype(F32)
    mine = jnp.sum(hit, axis=1, keepdims=True)
    mine = jnp.broadcast_to(mine, (TOK, SLOTS))
    row = lax.broadcasted_iota(jnp.int32, (TOK, TOK), 0)
    col = lax.broadcasted_iota(jnp.int32, (TOK, TOK), 1)
    before = (col < row).astype(BF)
    rank = jnp.dot(before, mine.astype(BF), preferred_element_type=F32)
    slot = lax.broadcasted_iota(jnp.int32, (TOK, SLOTS), 1).astype(F32)
    return jnp.where((mine > 0.5) & (jnp.abs(rank - slot) < 0.5), 1.0, 0.0)


def gather_kernel(
    prompt, ids, gain, gate, up, down,
    gate_out, up_out, down_out, rows,
    stg, stgd, abuf, dbuf,
    a_s, a_r, d_s, d_r, b_s, b_r, e_s, e_r, t_s, t_r, y_s, y_r,
):
    g, zl, y, x, c = place()
    me_t = x * 2 + c
    barrier = pltpu.get_barrier_semaphore()
    right = dev(g, zl, lax.rem(y + 1, 8), x, c)
    left = dev(g, zl, lax.rem(y + 7, 8), x, c)
    half = lax.div(y, 4)
    x1, c1 = served_by(g, x)
    ge = lax.div(x, 2)
    _, _, xe = home_of(ge, lax.rem(me_t, 4))

    @pl.loop(0, 32)
    def _(i):
        xs, ys = lax.div(i, 8), lax.rem(i, 8)

        @pl.when((xs != x) | (ys != y) | (half != c))
        def _():
            signal(barrier, dev(g, zl, ys, xs, half))

    @pl.loop(0, 8)
    def _(i):
        @pl.when(i != me_t)
        def _():
            signal(barrier, (g, zl * 8 + y, i))

        zs, w = lax.div(i, 2), lax.rem(i, 2)

        @pl.when((ge != g) | (zs != zl) | (xe != x) | (w != c))
        def _():
            signal(barrier, dev(ge, zs, y, xe, w))

    @pl.loop(1, 4)
    def _(j):
        signal(barrier, dev(g, lax.rem(zl + j, 4), y, x, c))

    signal(barrier, right)
    signal(barrier, left)

    chosen = choice_matrix(ids[...]).astype(BF)
    xf = prompt[...].astype(F32)
    normed = (xf * lax.rsqrt(jnp.mean(xf * xf, axis=1, keepdims=True) + NORM_EPS)).astype(BF)
    routed = lax.dot_general(chosen, normed, (((0,), (0,)), ((), ())), preferred_element_type=F32)
    rows[y, zl] = routed.astype(BF)

    @pl.loop(0, 4)
    def _(el):
        for h in range(2):
            stgd[el, h] = down[el, h * 128 : (h + 1) * 128, :].astype(BF)

    col = gain[...]

    @pl.loop(0, 4)
    def _(el):
        for k in range(4):
            cols = slice(k * 256, (k + 1) * 256)
            stg[0, el, k] = (gate[el, :, cols] * col).astype(BF)
            stg[1, el, k] = (up[el, :, cols] * col).astype(BF)

    same_half = jnp.where(half == c, 1, 0)
    own_b = jnp.where(ge == g, 1, 0) * (1 - c)
    pl.semaphore_wait(barrier, 32 - same_half + 7 + 8 - own_b + 3 + 2)

    def z_send(j):
        to = lax.rem(zl + j, 4)
        return rcopy(rows.at[y, zl], rows.at[y, zl], t_s.at[j], t_r.at[zl], dev(g, to, y, x, c))

    def r_send(s, q):
        at = lax.rem(y - s + 9, 8)
        return rcopy(rows.at[at, q], rows.at[at, q], y_s.at[0, s, q], y_r.at[0, s, q], right)

    def l_send(s, q):
        at = lax.rem(y + s + 7, 8)
        return rcopy(rows.at[at, q], rows.at[at, q], y_s.at[1, s, q], y_r.at[1, s, q], left)

    @pl.loop(1, 4)
    def _(j):
        z_send(j).start()

    def d_parts(i):
        el, h = lax.div(i, 2), lax.rem(i, 2)
        _, _, x2 = home_of(g, el)
        own = (x2 == x) & (h == c)
        dst = dbuf.at[:, pl.ds(pl.multiple_of(me_t * 256, 256), 256)]
        return own, stgd.at[el, h], dst, dev(g, zl, y, x2, h)

    @pl.loop(0, 8)
    def _(i):
        own, src, dst, to = d_parts(i)

        @pl.when(own)
        def _():
            pltpu.make_async_copy(src, dst, d_r).start()

        @pl.when(jnp.logical_not(own))
        def _():
            rcopy(src, dst, d_s.at[i], d_r, to).start()

    r_send(1, zl).start()
    l_send(1, zl).start()

    def a_parts(i):
        el, k, w = lax.div(i, 8), lax.rem(lax.div(i, 2), 4), lax.rem(i, 2)
        _, _, x2 = home_of(g, el)
        y2 = 4 * c + k
        own = (x2 == x) & (w == c) & (y2 == y)
        dst = abuf.at[x, pl.ds(pl.multiple_of(y * 64, 64), 64), :]
        return own, stg.at[w, el, k], dst, dev(g, zl, y2, x2, w)

    @pl.loop(0, 32)
    def _(i):
        own, src, dst, to = a_parts(i)

        @pl.when(own)
        def _():
            pltpu.make_async_copy(src, dst, a_r.at[x]).start()

        @pl.when(jnp.logical_not(own))
        def _():
            rcopy(src, dst, a_s.at[i], a_r.at[x], to).start()

    def e_parts(i):
        g2 = lax.rem(g + i, 2)
        own = (i == 0) & (x1 == x) & (c1 == c)
        dst = down_out.at[pl.ds(pl.multiple_of(c * 128, 128), 128), :]
        return own, dbuf, dst, dev(g2, zl, y, x1, c1)

    arrived(dbuf, d_r)

    @pl.loop(0, 2)
    def _(i):
        own, src, dst, to = e_parts(i)

        @pl.when(own)
        def _():
            pltpu.make_async_copy(src, dst, e_r.at[c]).start()

        @pl.when(jnp.logical_not(own))
        def _():
            rcopy(src, dst, e_s.at[i], e_r.at[c], to).start()

    @pl.loop(1, 4)
    def _(j):
        q = lax.rem(zl + j, 4)
        arrived(rows.at[y, q], t_r.at[q])
        r_send(1, q).start()
        l_send(1, q).start()

    def b_parts(i, out):
        xs, g2 = lax.div(i, 2), lax.rem(i, 2)
        own = (g2 == g) & (xs == zl) & (x1 == x) & (c1 == c)
        dst = out.at[pl.ds(pl.multiple_of(zl * 512, 512), 512), :]
        return own, abuf.at[xs], dst, dev(g2, xs, y, x1, c1)

    for w, out in ((0, gate_out), (1, up_out)):

        @pl.when(c == w)
        def _():
            @pl.loop(0, 8)
            def _(i):
                own, src, dst, to = b_parts(i, out)

                @pl.when(lax.rem(i, 2) == 0)
                def _():
                    arrived(src, a_r.at[lax.div(i, 2)])

                @pl.when(own)
                def _():
                    pltpu.make_async_copy(src, dst, b_r.at[w, zl]).start()

                @pl.when(jnp.logical_not(own))
                def _():
                    rcopy(src, dst, b_s.at[i], b_r.at[w, zl], to).start()

    def ring_step(s):
        @pl.loop(0, 4)
        def _(j):
            q = lax.rem(zl + j, 4)
            arrived(rows.at[lax.rem(y - s + 9, 8), q], y_r.at[0, s - 1, q])
            arrived(rows.at[lax.rem(y + s + 7, 8), q], y_r.at[1, s - 1, q])
            if s < 4:
                r_send(s, q).start()
                l_send(s, q).start()
            else:

                @pl.when(q < 2)
                def _():
                    r_send(s, q).start()

                @pl.when(q >= 2)
                def _():
                    l_send(s, q).start()

    for s in (2, 3, 4):
        ring_step(s)

    far = lax.rem(y + 4, 8)
    for q in range(4):
        arrived(rows.at[far, q], y_r.at[q // 2, 4, q])
    for q in range(4):
        arrived(gate_out.at[q * 512 : (q + 1) * 512, :], b_r.at[0, q])
        arrived(up_out.at[q * 512 : (q + 1) * 512, :], b_r.at[1, q])
    for h in range(2):
        arrived(down_out.at[h * 128 : (h + 1) * 128, :], e_r.at[h])

    @pl.loop(1, 4)
    def _(j):
        z_send(j).wait_send()

    @pl.loop(0, 8)
    def _(i):
        own, src, dst, to = d_parts(i)

        @pl.when(jnp.logical_not(own))
        def _():
            rcopy(src, dst, d_s.at[i], d_r, to).wait_send()

    @pl.loop(0, 32)
    def _(i):
        own, src, dst, to = a_parts(i)

        @pl.when(jnp.logical_not(own))
        def _():
            rcopy(src, dst, a_s.at[i], a_r.at[x], to).wait_send()

    @pl.loop(0, 2)
    def _(i):
        own, src, dst, to = e_parts(i)

        @pl.when(jnp.logical_not(own))
        def _():
            rcopy(src, dst, e_s.at[i], e_r.at[c], to).wait_send()

    @pl.loop(0, 8)
    def _(i):
        own, src, dst, to = b_parts(i, gate_out)

        @pl.when(jnp.logical_not(own))
        def _():
            rcopy(src, dst, b_s.at[i], b_r.at[0, zl], to).wait_send()

    for s in (1, 2, 3):

        @pl.loop(0, 4)
        def _(q):
            r_send(s, q).wait_send()
            l_send(s, q).wait_send()

    for q in range(2):
        r_send(4, q).wait_send()
        l_send(4, q + 2).wait_send()


def combine_kernel(
    part, ids, weights, mixed,
    keep, got, fin, gotz, sendc, gotc,
    y_s, y_r, z_s, z_r, c_s, c_r,
):
    g, zl, y, x, c = place()
    me_t = x * 2 + c
    barrier = pltpu.get_barrier_semaphore()
    right = dev(g, zl, lax.rem(y + 1, 8), x, c)
    left = dev(g, zl, lax.rem(y + 7, 8), x, c)
    signal(barrier, right)
    signal(barrier, left)

    @pl.loop(1, 4)
    def _(j):
        signal(barrier, dev(g, lax.rem(zl + j, 4), y, x, c))

    @pl.loop(1, 8)
    def _(j):
        signal(barrier, (g, zl * 8 + y, lax.rem(me_t + j, 8)))

    chosen = choice_matrix(ids[...])
    e = lax.axis_index("tp")
    wcol = jnp.sum(jnp.where(ids[...] == e, weights[...], 0.0), axis=1, keepdims=True)
    wrow = jnp.sum(chosen * wcol, axis=0, keepdims=True)
    eye = lax.broadcasted_iota(jnp.int32, (SLOTS, SLOTS), 0) == lax.broadcasted_iota(
        jnp.int32, (SLOTS, SLOTS), 1
    )
    wslot = jnp.sum(jnp.where(eye, jnp.broadcast_to(wrow, (SLOTS, SLOTS)), 0.0), axis=1, keepdims=True)

    pl.semaphore_wait(barrier, 12)

    def target(way, s):
        return lax.rem(y + 5 - s, 8) if way == 0 else lax.rem(y + 3 + s, 8)

    def send(way, s, q, src):
        return rcopy(
            src, got.at[way, s - 1, q], y_s.at[way, s - 1, q], y_r.at[way, s - 1, q], (right, left)[way]
        )

    def first_hand(way, s, q):
        return s == 1 or (s == 2 and q // 2 != way)

    def source(way, s, q):
        if first_hand(way, s, q):
            return part.at[target(way, s), q]
        return keep.at[way, s - 2, q]

    for q in range(2):
        for way in range(2):
            send(way, 1, q + 2 * way, source(way, 1, q + 2 * way)).start()
    for q in range(2):
        for way in range(2):
            other = q + 2 * (1 - way)
            send(way, 2, other, source(way, 2, other)).start()
    for s in (2, 3, 4):
        order = (0, 1) if s == 2 else (2, 3, 0, 1)
        for j in order:
            for way in range(2):
                q = (j + 2 * way) % 4
                arrived(got.at[way, s - 2, q], y_r.at[way, s - 2, q])
                total = part[target(way, s), q].astype(F32) + got[way, s - 2, q].astype(F32)
                keep[way, s - 2, q] = total.astype(BF)
                send(way, s, q, source(way, s, q)).start()

    def z_send(q):
        return rcopy(fin.at[q], gotz.at[zl], z_s.at[q], z_r.at[zl], dev(g, q, y, x, c))

    for q in (2, 0, 3, 1):
        for way in range(2):
            arrived(got.at[way, 3, q], y_r.at[way, 3, q])
        total = part[y, q].astype(F32) + got[0, 3, q].astype(F32) + got[1, 3, q].astype(F32)
        fin[q] = total.astype(BF)

        @pl.when(zl != q)
        def _():
            z_send(q).start()

    out = fin[zl].astype(F32)
    for j in range(1, 4):
        q = lax.rem(zl + j, 4)
        arrived(gotz.at[q], z_r.at[q])
        out = out + gotz[q].astype(F32)

    term = (out * wslot).astype(BF)
    spread = jnp.dot(chosen.astype(BF), term, preferred_element_type=F32).astype(BF)
    for t in range(8):
        sendc[t] = spread[t * 16 : (t + 1) * 16, :]

    def c_send(j):
        t = lax.rem(me_t + j, 8)
        return rcopy(sendc.at[t], gotc.at[me_t], c_s.at[j], c_r.at[me_t], (g, zl * 8 + y, t))

    @pl.loop(1, 8)
    def _(j):
        c_send(j).start()

    total = sendc[me_t].astype(F32)
    for j in range(1, 8):
        t = lax.rem(me_t + j, 8)
        arrived(gotc.at[t], c_r.at[t])
        total = total + gotc[t].astype(F32)
    mixed[...] = total.astype(BF)

    for s in (1, 2, 3, 4):
        for q in range(4):
            for way in range(2):
                if s > 1 or q // 2 == way:
                    send(way, s, q, source(way, s, q)).wait_send()
    for q in range(4):

        @pl.when(zl != q)
        def _():
            z_send(q).wait_send()

    @pl.loop(1, 8)
    def _(j):
        c_send(j).wait_send()


VM = pl.BlockSpec(memory_space=pltpu.VMEM)
DMA = pltpu.SemaphoreType.DMA


def body(prompt, expert_ids, route_weights, gate_master, up_master, down_master, ffn_gain):
    gate, up, down, rows = pl.pallas_call(
        gather_kernel,
        out_shape=(
            jax.ShapeDtypeStruct((D, 256), BF),
            jax.ShapeDtypeStruct((D, 256), BF),
            jax.ShapeDtypeStruct((256, D), BF),
            jax.ShapeDtypeStruct((8, 4, SLOTS, D), BF),
        ),
        in_specs=[VM] * 6,
        out_specs=(VM,) * 4,
        scratch_shapes=[
            pltpu.VMEM((2, 4, 4, 64, 256), BF),
            pltpu.VMEM((4, 2, 128, 256), BF),
            pltpu.VMEM((4, 512, 256), BF),
            pltpu.VMEM((128, D), BF),
            DMA((32,)),
            DMA((4,)),
            DMA((8,)),
            DMA,
            DMA((8,)),
            DMA((2, 4)),
            DMA((2,)),
            DMA((2,)),
            DMA((4,)),
            DMA((4,)),
            DMA((2, 5, 4)),
            DMA((2, 5, 4)),
        ],
        compiler_params=pltpu.CompilerParams(
            collective_id=0, has_side_effects=True, vmem_limit_bytes=40 << 20
        ),
        name="gather",
    )(prompt, expert_ids, ffn_gain[:, None], gate_master, up_master, down_master)
    piece = rows.reshape(8 * 4 * SLOTS, D)
    gate_part = jnp.dot(piece, gate, preferred_element_type=F32)
    up_part = jnp.dot(piece, up, preferred_element_type=F32)
    hidden = (jax.nn.silu(gate_part) * up_part).astype(BF)
    part = jnp.dot(hidden, down, preferred_element_type=F32).astype(BF)
    mixed = pl.pallas_call(
        combine_kernel,
        out_shape=jax.ShapeDtypeStruct((16, D), BF),
        in_specs=[VM] * 3,
        out_specs=VM,
        scratch_shapes=[
            pltpu.VMEM((2, 3, 4, SLOTS, D), BF),
            pltpu.VMEM((2, 4, 4, SLOTS, D), BF),
            pltpu.VMEM((4, SLOTS, D), BF),
            pltpu.VMEM((4, SLOTS, D), BF),
            pltpu.VMEM((8, 16, D), BF),
            pltpu.VMEM((8, 16, D), BF),
            DMA((2, 4, 4)),
            DMA((2, 4, 4)),
            DMA((4,)),
            DMA((4,)),
            DMA((8,)),
            DMA((8,)),
        ],
        compiler_params=pltpu.CompilerParams(
            collective_id=1, has_side_effects=True, vmem_limit_bytes=40 << 20
        ),
        name="combine",
    )(part.reshape(8, 4, SLOTS, D), expert_ids, route_weights)
    return gate[None], up[None], down[None], mixed


def solution(mesh):
    return jax.shard_map(
        body,
        mesh=mesh,
        in_specs=(
            P(("gr", "fs"), None),
            P(("gr", "fs"), None),
            P(("gr", "fs"), None),
            P("gr", "fs", "tp"),
            P("gr", "fs", "tp"),
            P("gr", "fs", "tp"),
            P("fs"),
        ),
        out_specs=(
            P("tp", None, "fs"),
            P("tp", None, "fs"),
            P("tp", "fs", None),
            P(("gr", "fs", "tp"), None),
        ),
        check_vma=False,
    )
```

```python
import jax
import jax.numpy as jnp
from jax import lax
from jax.experimental import pallas as pl
from jax.experimental.pallas import tpu as pltpu
from jax.sharding import PartitionSpec as P

EXPERTS = 8
SLOTS = 32
TOK = 128
D = 2048
NORM_EPS = 1e-06
MESH = pl.DeviceIdType.MESH
BF = jnp.bfloat16
F32 = jnp.float32


def place():
    g, f, t = lax.axis_index("gr"), lax.axis_index("fs"), lax.axis_index("tp")
    return g, lax.div(f, 8), lax.rem(f, 8), lax.div(t, 2), lax.rem(t, 2)


def dev(g, zl, y, x, c):
    return (g, zl * 8 + y, x * 2 + c)


def signal(sem, where):
    pl.semaphore_signal(sem, inc=1, device_id=where, device_id_type=MESH)


def rcopy(src, dst, ssem, rsem, where):
    return pltpu.make_async_remote_copy(
        src_ref=src, dst_ref=dst, send_sem=ssem, recv_sem=rsem, device_id=where, device_id_type=MESH
    )


def arrived(buf, sem):
    pltpu.make_async_copy(buf, buf, sem).wait()


def home_of(g, el):
    odd = lax.rem(el, 2)
    x1 = 2 * g + lax.div(el, 2)
    return x1, odd, x1 * (1 - odd) + (3 - x1) * odd


def served_by(g, x):
    h = lax.div(x, 2)
    c1 = h + g - 2 * h * g
    return x * (1 - c1) + (3 - x) * c1, c1


def choice_matrix(ids):
    e = lax.axis_index("tp")
    mine = jnp.sum((ids == e).astype(F32), axis=0, keepdims=True)
    mine = jnp.broadcast_to(mine, (SLOTS, TOK))
    row = lax.broadcasted_iota(jnp.int32, (TOK, TOK), 0)
    col = lax.broadcasted_iota(jnp.int32, (TOK, TOK), 1)
    before = (row < col).astype(BF)
    rank = jnp.dot(mine.astype(BF), before, preferred_element_type=F32)
    slot = lax.broadcasted_iota(jnp.int32, (SLOTS, TOK), 0).astype(F32)
    return jnp.where((mine > 0.5) & (jnp.abs(rank - slot) < 0.5), 1.0, 0.0)


def kernel(
    prompt_h, gate_h, up_h, down_h, ids, weights, gain,
    gate_out, up_out, down_out, mixed,
    prompt, gate, up, down, stg, stgd, abuf, dbuf, rows,
    hid, part, keep, got, fin, gotz, sendc, gotc,
    in_s, a_s, a_r, d_s, d_r, b_s, b_r, e_s, e_r, t_s, t_r, y_s, y_r,
    p_s, p_r, z_s, z_r, c_s, c_r,
):
    loads = [
        pltpu.make_async_copy(src, dst, in_s.at[i])
        for i, (src, dst) in enumerate(
            ((prompt_h, prompt), (down_h, down), (gate_h, gate), (up_h, up))
        )
    ]
    for load in loads:
        load.start()
    g, zl, y, x, c = place()
    me_t = x * 2 + c
    barrier = pltpu.get_barrier_semaphore()
    right = dev(g, zl, lax.rem(y + 1, 8), x, c)
    left = dev(g, zl, lax.rem(y + 7, 8), x, c)
    half = lax.div(y, 4)
    x1, c1 = served_by(g, x)
    ge = lax.div(x, 2)
    _, _, xe = home_of(ge, lax.rem(me_t, 4))

    @pl.loop(0, 32)
    def _(i):
        xs, ys = lax.div(i, 8), lax.rem(i, 8)

        @pl.when((xs != x) | (ys != y) | (half != c))
        def _():
            signal(barrier, dev(g, zl, ys, xs, half))

    @pl.loop(0, 8)
    def _(i):
        @pl.when(i != me_t)
        def _():
            signal(barrier, (g, zl * 8 + y, i))

        zs, w = lax.div(i, 2), lax.rem(i, 2)

        @pl.when((ge != g) | (zs != zl) | (xe != x) | (w != c))
        def _():
            signal(barrier, dev(ge, zs, y, xe, w))

    @pl.loop(1, 4)
    def _(j):
        signal(barrier, dev(g, lax.rem(zl + j, 4), y, x, c))

    signal(barrier, right)
    signal(barrier, left)

    choice = choice_matrix(ids[...])
    wslot = jnp.sum(
        choice
        * jnp.sum(jnp.where(ids[...] == me_t, weights[...], 0.0), axis=0, keepdims=True),
        axis=1,
        keepdims=True,
    )
    chosen = choice.astype(BF)
    loads[0].wait()
    xf = prompt[...].astype(F32)
    normed = (xf * lax.rsqrt(jnp.mean(xf * xf, axis=1, keepdims=True) + NORM_EPS)).astype(BF)
    rows[y, zl] = jnp.dot(chosen, normed, preferred_element_type=F32).astype(BF)

    loads[1].wait()

    @pl.loop(0, 4)
    def _(el):
        for h in range(2):
            stgd[el, h] = down[el, h * 128 : (h + 1) * 128, :].astype(BF)

    eye = lax.broadcasted_iota(jnp.int32, (64, 64), 0) == lax.broadcasted_iota(jnp.int32, (64, 64), 1)
    col = jnp.sum(
        jnp.where(eye, jnp.broadcast_to(gain[...], (64, 64)), 0.0), axis=1, keepdims=True
    )
    loads[2].wait()
    loads[3].wait()

    @pl.loop(0, 4)
    def _(el):
        for k in range(4):
            cols = slice(k * 256, (k + 1) * 256)
            stg[0, el, k] = (gate[el, :, cols] * col).astype(BF)
            stg[1, el, k] = (up[el, :, cols] * col).astype(BF)

    same_half = jnp.where(half == c, 1, 0)
    own_b = jnp.where(ge == g, 1, 0) * (1 - c)
    pl.semaphore_wait(barrier, 32 - same_half + 7 + 8 - own_b + 3 + 2)

    def z_send(j):
        to = lax.rem(zl + j, 4)
        return rcopy(rows.at[y, zl], rows.at[y, zl], t_s.at[j], t_r.at[zl], dev(g, to, y, x, c))

    def r_send(s, q):
        at = lax.rem(y - s + 9, 8)
        return rcopy(rows.at[at, q], rows.at[at, q], y_s.at[0, s, q], y_r.at[0, s, q], right)

    def l_send(s, q):
        at = lax.rem(y + s + 7, 8)
        return rcopy(rows.at[at, q], rows.at[at, q], y_s.at[1, s, q], y_r.at[1, s, q], left)

    @pl.loop(1, 4)
    def _(j):
        z_send(j).start()

    def collected(x2):
        x0, c0 = served_by(g, x2)
        return 2 * (x0 - 2 * g) + c0

    def d_parts(i):
        x2, h = lax.rem(x + 1 + lax.div(i, 2), 4), lax.rem(i, 2)
        own = (x2 == x) & (h == c)
        dst = dbuf.at[x, :, pl.ds(pl.multiple_of(c * 256, 256), 256)]
        return own, stgd.at[collected(x2), h], dst, dev(g, zl, y, x2, h)

    @pl.loop(0, 8)
    def _(i):
        own, src, dst, to = d_parts(i)

        @pl.when(own)
        def _():
            pltpu.make_async_copy(src, dst, d_r.at[x]).start()

        @pl.when(jnp.logical_not(own))
        def _():
            rcopy(src, dst, d_s.at[i], d_r.at[x], to).start()

    r_send(1, zl).start()
    l_send(1, zl).start()

    def a_parts(i):
        k, w = lax.rem(y + lax.rem(lax.div(i, 2), 4), 4), lax.rem(i, 2)
        x2 = lax.rem(x + 5 + lax.div(i, 8) - zl, 4)
        el, y2 = collected(x2), 4 * c + k
        own = (x2 == x) & (w == c) & (y2 == y)
        dst = abuf.at[x, pl.ds(pl.multiple_of(y * 64, 64), 64), :]
        return own, stg.at[w, el, k], dst, dev(g, zl, y2, x2, w)

    @pl.loop(0, 32)
    def _(i):
        own, src, dst, to = a_parts(i)

        @pl.when(own)
        def _():
            pltpu.make_async_copy(src, dst, a_r.at[x]).start()

        @pl.when(jnp.logical_not(own))
        def _():
            rcopy(src, dst, a_s.at[i], a_r.at[x], to).start()

    def e_parts(i):
        j, g2 = lax.div(i, 2), lax.rem(g + 1 + i, 2)
        own = (g2 == g) & (x1 == x) & (c1 == c)
        dst = down_out.at[
            pl.ds(pl.multiple_of(c * 128, 128), 128), pl.ds(pl.multiple_of(j * 512, 512), 512)
        ]
        return own, dbuf.at[j], dst, dev(g2, zl, y, x1, c1), e_r.at[c, j]

    def e_start(first):
        @pl.loop(first, first + 4)
        def _(i):
            own, src, dst, to, sem = e_parts(i)

            @pl.when(lax.rem(i, 2) == 0)
            def _():
                arrived(src, d_r.at[lax.div(i, 2)])

            @pl.when(own)
            def _():
                pltpu.make_async_copy(src, dst, sem).start()

            @pl.when(jnp.logical_not(own))
            def _():
                rcopy(src, dst, e_s.at[i], sem, to).start()

    e_start(0)

    def b_parts(i, out):
        xs, g2 = lax.rem(x + 7 - lax.div(i, 2) + zl, 4), lax.rem(g + 1 + i, 2)
        own = (g2 == g) & (xs == zl) & (x1 == x) & (c1 == c)
        dst = out.at[pl.ds(pl.multiple_of(zl * 512, 512), 512), :]
        return own, abuf.at[xs], dst, dev(g2, xs, y, x1, c1)

    def b_step(m):
        xs = lax.rem(x + 7 - m + zl, 4)
        arrived(abuf.at[xs], a_r.at[xs])
        for w, out in ((0, gate_out), (1, up_out)):

            @pl.when(c == w)
            def _():
                @pl.loop(2 * m, 2 * m + 2)
                def _(i):
                    own, src, dst, to = b_parts(i, out)

                    @pl.when(own)
                    def _():
                        pltpu.make_async_copy(src, dst, b_r.at[w, zl]).start()

                    @pl.when(jnp.logical_not(own))
                    def _():
                        rcopy(src, dst, b_s.at[i], b_r.at[w, zl], to).start()

    def nth(j):
        return lax.rem(zl + 4 + j * (1 - 2 * lax.div(zl, 2)), 4)

    for m in range(4):
        b_step(m)
        if m < 3:
            q = nth(m + 1)
            arrived(rows.at[y, q], t_r.at[q])
            r_send(1, q).start()
            l_send(1, q).start()

    e_start(4)

    def ring_step(s):
        @pl.loop(0, 4)
        def _(j):
            q = nth(j)
            arrived(rows.at[lax.rem(y - s + 9, 8), q], y_r.at[0, s - 1, q])
            arrived(rows.at[lax.rem(y + s + 7, 8), q], y_r.at[1, s - 1, q])
            if s < 4:
                r_send(s, q).start()
                l_send(s, q).start()
            else:

                @pl.when(q < 2)
                def _():
                    r_send(s, q).start()

                @pl.when(q >= 2)
                def _():
                    l_send(s, q).start()

    for s in (2, 3, 4):
        ring_step(s)

    far = lax.rem(y + 4, 8)
    for q in range(4):
        arrived(rows.at[far, q], y_r.at[q // 2, 4, q])
    for q in range(4):
        arrived(gate_out.at[q * 512 : (q + 1) * 512, :], b_r.at[0, q])
        arrived(up_out.at[q * 512 : (q + 1) * 512, :], b_r.at[1, q])
    @pl.loop(0, 4)
    def _(i):
        x_in = rows[pl.ds(2 * i, 2)].reshape(8 * SLOTS, D)
        gate_part = jnp.dot(x_in, gate_out[...], preferred_element_type=F32)
        up_part = jnp.dot(x_in, up_out[...], preferred_element_type=F32)
        hid[i] = (gate_part / (1.0 + jnp.exp(-gate_part)) * up_part).astype(BF)

    def target(way, s):
        return lax.rem(y + 5 - s, 8) if way == 0 else lax.rem(y + 3 + s, 8)

    def send(way, s, q, src):
        return rcopy(
            src, got.at[way, s - 1, q], p_s.at[way, s - 1, q], p_r.at[way, s - 1, q], (right, left)[way]
        )

    def first_hand(way, s, q):
        return s == 1 or (s == 2 and q // 2 != way)

    def source(way, s, q):
        if first_hand(way, s, q):
            return part.at[target(way, s), q]
        return keep.at[way, s - 2, q]

    def make(q):
        for h in range(2):
            at = down_out.at[h * 128 : (h + 1) * 128, q * 512 : (q + 1) * 512]
            arrived(at, e_r.at[h, q])

        @pl.loop(0, 4)
        def _(i):
            made = jnp.dot(
                hid[i], down_out[:, q * 512 : (q + 1) * 512], preferred_element_type=F32
            ).astype(BF)
            part[2 * i, q] = made[:128]
            part[2 * i + 1, q] = made[128:]

        send(q // 2, 1, q, source(q // 2, 1, q)).start()
        send(1 - q // 2, 2, q, source(1 - q // 2, 2, q)).start()

    def pass_on(way, s, q):
        arrived(got.at[way, s - 2, q], p_r.at[way, s - 2, q])
        total = part[target(way, s), q].astype(F32) + got[way, s - 2, q].astype(F32)
        keep[way, s - 2, q] = total.astype(BF)
        send(way, s, q, source(way, s, q)).start()

    for q in (0, 1, 2, 3):
        make(q)
    for s, order in ((2, (0, 1)), (3, (2, 3, 0, 1)), (4, (2, 0, 3, 1))):
        for j in order:
            for way in range(2):
                pass_on(way, s, (j + 2 * way) % 4)

    def f_send(q, j):
        to = lax.rem(zl + j, 4)
        src = fin.at[q, pl.ds(pl.multiple_of(to * 32, 32), 32), :]
        return rcopy(src, gotz.at[q, zl], z_s.at[q, j], z_r.at[q, zl], dev(g, to, y, x, c))

    def finish(q):
        for way in range(2):
            arrived(got.at[way, 3, q], p_r.at[way, 3, q])
        total = part[y, q].astype(F32) + got[0, 3, q].astype(F32) + got[1, 3, q].astype(F32)
        fin[q] = total.astype(BF)

        @pl.loop(1, 4)
        def _(j):
            f_send(q, j).start()

    def c_send(q, j):
        t = lax.rem(me_t + j, 8)
        return rcopy(
            sendc.at[q, t], gotc.at[q, me_t], c_s.at[q, j], c_r.at[q, me_t], (g, zl * 8 + y, t)
        )

    def spread(q):
        out = fin[q, pl.ds(pl.multiple_of(zl * 32, 32), 32), :].astype(F32)
        for j in range(1, 4):
            k = lax.rem(zl + j, 4)
            arrived(gotz.at[q, k], z_r.at[q, k])
            out = out + gotz[q, k].astype(F32)
        term = (out * wslot).astype(BF)
        wide = lax.dot_general(
            chosen, term, (((0,), (0,)), ((), ())), preferred_element_type=F32
        ).astype(BF)
        for t in range(8):
            sendc[q, t] = wide[t * 16 : (t + 1) * 16, :]

        @pl.loop(1, 8)
        def _(j):
            c_send(q, j).start()

    def settle(q):
        total = sendc[q, me_t].astype(F32)
        for j in range(1, 8):
            t = lax.rem(me_t + j, 8)
            arrived(gotc.at[q, t], c_r.at[q, t])
            total = total + gotc[q, t].astype(F32)
        mixed[:, q * 512 : (q + 1) * 512] = total.astype(BF)

    @pl.loop(1, 4)
    def _(j):
        z_send(j).wait_send()

    @pl.loop(0, 8)
    def _(i):
        own, src, dst, to = d_parts(i)

        @pl.when(jnp.logical_not(own))
        def _():
            rcopy(src, dst, d_s.at[i], d_r.at[x], to).wait_send()

    @pl.loop(0, 32)
    def _(i):
        own, src, dst, to = a_parts(i)

        @pl.when(jnp.logical_not(own))
        def _():
            rcopy(src, dst, a_s.at[i], a_r.at[x], to).wait_send()

    @pl.loop(0, 8)
    def _(i):
        own, src, dst, to, sem = e_parts(i)

        @pl.when(jnp.logical_not(own))
        def _():
            rcopy(src, dst, e_s.at[i], sem, to).wait_send()

    @pl.loop(0, 8)
    def _(i):
        own, src, dst, to = b_parts(i, gate_out)

        @pl.when(jnp.logical_not(own))
        def _():
            rcopy(src, dst, b_s.at[i], b_r.at[0, zl], to).wait_send()

    for s in (1, 2, 3):

        @pl.loop(0, 4)
        def _(q):
            r_send(s, q).wait_send()
            l_send(s, q).wait_send()

    for q in range(2):
        r_send(4, q).wait_send()
        l_send(4, q + 2).wait_send()

    for s in (1, 2, 3):
        for q in range(4):
            for way in range(2):
                if s > 1 or q // 2 == way:
                    send(way, s, q, source(way, s, q)).wait_send()

    for q in (0, 2, 1, 3):
        finish(q)
    for q in (0, 2, 1, 3):
        spread(q)
    for q in (0, 2, 1, 3):
        settle(q)

    for q in range(4):
        for way in range(2):
            send(way, 4, q, source(way, 4, q)).wait_send()

        @pl.loop(1, 4)
        def _(j):
            f_send(q, j).wait_send()

        @pl.loop(1, 8)
        def _(j):
            c_send(q, j).wait_send()


VM = pl.BlockSpec(memory_space=pltpu.VMEM)
HB = pl.BlockSpec(memory_space=pltpu.MemorySpace.HBM)
DMA = pltpu.SemaphoreType.DMA


def body(prompt, expert_ids, route_weights, gate_master, up_master, down_master, ffn_gain):
    gate, up, down, mixed = pl.pallas_call(
        kernel,
        out_shape=(
            jax.ShapeDtypeStruct((D, 256), BF),
            jax.ShapeDtypeStruct((D, 256), BF),
            jax.ShapeDtypeStruct((256, D), BF),
            jax.ShapeDtypeStruct((16, D), BF),
        ),
        in_specs=[HB] * 4 + [VM] * 3,
        out_specs=(VM,) * 4,
        scratch_shapes=[
            pltpu.VMEM((TOK, D), BF),
            pltpu.VMEM((4, 64, 1024), F32),
            pltpu.VMEM((4, 64, 1024), F32),
            pltpu.VMEM((4, 256, 256), F32),
            pltpu.VMEM((2, 4, 4, 64, 256), BF),
            pltpu.VMEM((4, 2, 128, 256), BF),
            pltpu.VMEM((4, 512, 256), BF),
            pltpu.VMEM((4, 128, 512), BF),
            pltpu.VMEM((8, 4, SLOTS, D), BF),
            pltpu.VMEM((4, 256, 256), BF),
            pltpu.VMEM((8, 4, 128, 512), BF),
            pltpu.VMEM((2, 3, 4, 128, 512), BF),
            pltpu.VMEM((2, 4, 4, 128, 512), BF),
            pltpu.VMEM((4, 128, 512), BF),
            pltpu.VMEM((4, 4, SLOTS, 512), BF),
            pltpu.VMEM((4, 8, 16, 512), BF),
            pltpu.VMEM((4, 8, 16, 512), BF),
            DMA((4,)),
            DMA((32,)),
            DMA((4,)),
            DMA((8,)),
            DMA((4,)),
            DMA((8,)),
            DMA((2, 4)),
            DMA((8,)),
            DMA((2, 4)),
            DMA((4,)),
            DMA((4,)),
            DMA((2, 5, 4)),
            DMA((2, 5, 4)),
            DMA((2, 4, 4)),
            DMA((2, 4, 4)),
            DMA((4, 4)),
            DMA((4, 4)),
            DMA((4, 8)),
            DMA((4, 8)),
        ],
        compiler_params=pltpu.CompilerParams(
            collective_id=0, has_side_effects=True, vmem_limit_bytes=36 << 20
        ),
        name="serve",
    )(
        *(
            pltpu.with_memory_space_constraint(v, pltpu.MemorySpace.HBM)
            for v in (prompt, gate_master, up_master, down_master)
        ),
        expert_ids.T, route_weights.T, ffn_gain[None],
    )
    return gate[None], up[None], down[None], mixed


def solution(mesh):
    return jax.shard_map(
        body,
        mesh=mesh,
        in_specs=(
            P(("gr", "fs"), None),
            P(("gr", "fs"), None),
            P(("gr", "fs"), None),
            P("gr", "fs", "tp"),
            P("gr", "fs", "tp"),
            P("gr", "fs", "tp"),
            P("fs"),
        ),
        out_specs=(
            P("tp", None, "fs"),
            P("tp", None, "fs"),
            P("tp", "fs", None),
            P(("gr", "fs", "tp"), None),
        ),
        check_vma=False,
    )
```

```python
import jax
import jax.numpy as jnp
from jax import lax
from jax.experimental import pallas as pl
from jax.experimental.pallas import tpu as pltpu
from jax.sharding import PartitionSpec as P

EXPERTS = 8
SLOTS = 32
TOK = 128
D = 2048
NORM_EPS = 1e-06
MESH = pl.DeviceIdType.MESH
BF = jnp.bfloat16
F32 = jnp.float32


def place():
    g, f, t = lax.axis_index("gr"), lax.axis_index("fs"), lax.axis_index("tp")
    return g, lax.div(f, 8), lax.rem(f, 8), lax.div(t, 2), lax.rem(t, 2)


def dev(g, zl, y, x, c):
    return (g, zl * 8 + y, x * 2 + c)


def signal(sem, where):
    pl.semaphore_signal(sem, inc=1, device_id=where, device_id_type=MESH)


def rcopy(src, dst, ssem, rsem, where):
    return pltpu.make_async_remote_copy(
        src_ref=src, dst_ref=dst, send_sem=ssem, recv_sem=rsem, device_id=where, device_id_type=MESH
    )


def arrived(buf, sem):
    pltpu.make_async_copy(buf, buf, sem).wait()


def home_of(g, el):
    odd = lax.rem(el, 2)
    x1 = 2 * g + lax.div(el, 2)
    return x1, odd, x1 * (1 - odd) + (3 - x1) * odd


def served_by(g, x):
    h = lax.div(x, 2)
    c1 = h + g - 2 * h * g
    return x * (1 - c1) + (3 - x) * c1, c1


def choice_matrix(ids):
    e = lax.axis_index("tp")
    mine = jnp.sum((ids == e).astype(F32), axis=0, keepdims=True)
    mine = jnp.broadcast_to(mine, (SLOTS, TOK))
    row = lax.broadcasted_iota(jnp.int32, (TOK, TOK), 0)
    col = lax.broadcasted_iota(jnp.int32, (TOK, TOK), 1)
    before = (row < col).astype(BF)
    rank = jnp.dot(mine.astype(BF), before, preferred_element_type=F32)
    slot = lax.broadcasted_iota(jnp.int32, (SLOTS, TOK), 0).astype(F32)
    return jnp.where((mine > 0.5) & (jnp.abs(rank - slot) < 0.5), 1.0, 0.0)


def kernel(
    prompt_h, gate_h, up_h, down_h, ids, weights, gain,
    gate_out, up_out, down_out, mixed,
    prompt, gate, up, down, stg, stgd, abuf, dbuf, rows,
    acc, hid, part, keep, got, fin, gotz, sendc, gotc,
    in_s, a_s, a_r, d_s, d_r, b_s, b_r, e_s, e_r, t_s, t_r, y_s, y_r,
    p_s, p_r, z_s, z_r, c_s, c_r,
):
    loads = [
        pltpu.make_async_copy(src, dst, in_s.at[i])
        for i, (src, dst) in enumerate(
            ((prompt_h, prompt), (down_h, down), (gate_h, gate), (up_h, up))
        )
    ]
    for load in loads:
        load.start()
    g, zl, y, x, c = place()
    me_t = x * 2 + c
    barrier = pltpu.get_barrier_semaphore()
    right = dev(g, zl, lax.rem(y + 1, 8), x, c)
    left = dev(g, zl, lax.rem(y + 7, 8), x, c)
    half = lax.div(y, 4)
    x1, c1 = served_by(g, x)
    ge = lax.div(x, 2)
    _, _, xe = home_of(ge, lax.rem(me_t, 4))

    @pl.loop(0, 32)
    def _(i):
        xs, ys = lax.div(i, 8), lax.rem(i, 8)

        @pl.when((xs != x) | (ys != y) | (half != c))
        def _():
            signal(barrier, dev(g, zl, ys, xs, half))

    @pl.loop(0, 8)
    def _(i):
        @pl.when(i != me_t)
        def _():
            signal(barrier, (g, zl * 8 + y, i))

        zs, w = lax.div(i, 2), lax.rem(i, 2)

        @pl.when((ge != g) | (zs != zl) | (xe != x) | (w != c))
        def _():
            signal(barrier, dev(ge, zs, y, xe, w))

    @pl.loop(1, 4)
    def _(j):
        signal(barrier, dev(g, lax.rem(zl + j, 4), y, x, c))

    signal(barrier, right)
    signal(barrier, left)

    choice = choice_matrix(ids[...])
    wslot = jnp.sum(
        choice
        * jnp.sum(jnp.where(ids[...] == me_t, weights[...], 0.0), axis=0, keepdims=True),
        axis=1,
        keepdims=True,
    )
    chosen = choice.astype(BF)
    loads[0].wait()
    xf = prompt[...].astype(F32)
    normed = (xf * lax.rsqrt(jnp.mean(xf * xf, axis=1, keepdims=True) + NORM_EPS)).astype(BF)
    rows[y, zl] = jnp.dot(chosen, normed, preferred_element_type=F32).astype(BF)

    loads[1].wait()

    @pl.loop(0, 4)
    def _(el):
        for h in range(2):
            stgd[el, h] = down[el, h * 128 : (h + 1) * 128, :].astype(BF)

    eye = lax.broadcasted_iota(jnp.int32, (64, 64), 0) == lax.broadcasted_iota(jnp.int32, (64, 64), 1)
    col = jnp.sum(
        jnp.where(eye, jnp.broadcast_to(gain[...], (64, 64)), 0.0), axis=1, keepdims=True
    )
    loads[2].wait()
    loads[3].wait()

    @pl.loop(0, 4)
    def _(el):
        for k in range(4):
            cols = slice(k * 256, (k + 1) * 256)
            stg[0, el, k] = (gate[el, :, cols] * col).astype(BF)
            stg[1, el, k] = (up[el, :, cols] * col).astype(BF)

    same_half = jnp.where(half == c, 1, 0)
    own_b = jnp.where(ge == g, 1, 0) * (1 - c)
    pl.semaphore_wait(barrier, 32 - same_half + 7 + 8 - own_b + 3 + 2)

    def z_send(j):
        to = lax.rem(zl + j, 4)
        return rcopy(rows.at[y, zl], rows.at[y, zl], t_s.at[j], t_r.at[zl], dev(g, to, y, x, c))

    def r_send(s, q):
        at = lax.rem(y - s + 9, 8)
        return rcopy(rows.at[at, q], rows.at[at, q], y_s.at[0, s, q], y_r.at[0, s, q], right)

    def l_send(s, q):
        at = lax.rem(y + s + 7, 8)
        return rcopy(rows.at[at, q], rows.at[at, q], y_s.at[1, s, q], y_r.at[1, s, q], left)

    @pl.loop(1, 4)
    def _(j):
        z_send(j).start()

    def collected(x2):
        x0, c0 = served_by(g, x2)
        return 2 * (x0 - 2 * g) + c0

    def d_parts(i):
        x2, h = lax.rem(x + 1 + lax.div(i, 2), 4), lax.rem(i, 2)
        own = (x2 == x) & (h == c)
        dst = dbuf.at[x, :, pl.ds(pl.multiple_of(c * 256, 256), 256)]
        return own, stgd.at[collected(x2), h], dst, dev(g, zl, y, x2, h)

    @pl.loop(0, 8)
    def _(i):
        own, src, dst, to = d_parts(i)

        @pl.when(own)
        def _():
            pltpu.make_async_copy(src, dst, d_r.at[x]).start()

        @pl.when(jnp.logical_not(own))
        def _():
            rcopy(src, dst, d_s.at[i], d_r.at[x], to).start()

    r_send(1, zl).start()
    l_send(1, zl).start()

    def a_parts(i):
        k, w = lax.rem(y + lax.rem(lax.div(i, 2), 4), 4), lax.rem(i, 2)
        x2 = lax.rem(x + 5 + lax.div(i, 8) - zl, 4)
        el, y2 = collected(x2), 4 * c + k
        own = (x2 == x) & (w == c) & (y2 == y)
        dst = abuf.at[x, pl.ds(pl.multiple_of(y * 64, 64), 64), :]
        return own, stg.at[w, el, k], dst, dev(g, zl, y2, x2, w)

    @pl.loop(0, 32)
    def _(i):
        own, src, dst, to = a_parts(i)

        @pl.when(own)
        def _():
            pltpu.make_async_copy(src, dst, a_r.at[x]).start()

        @pl.when(jnp.logical_not(own))
        def _():
            rcopy(src, dst, a_s.at[i], a_r.at[x], to).start()

    def e_parts(i):
        j, g2 = lax.div(i, 2), lax.rem(g + 1 + i, 2)
        own = (g2 == g) & (x1 == x) & (c1 == c)
        dst = down_out.at[
            pl.ds(pl.multiple_of(c * 128, 128), 128), pl.ds(pl.multiple_of(j * 512, 512), 512)
        ]
        return own, dbuf.at[j], dst, dev(g2, zl, y, x1, c1), e_r.at[c, j]

    def e_start(first):
        @pl.loop(first, first + 4)
        def _(i):
            own, src, dst, to, sem = e_parts(i)

            @pl.when(lax.rem(i, 2) == 0)
            def _():
                arrived(src, d_r.at[lax.div(i, 2)])

            @pl.when(own)
            def _():
                pltpu.make_async_copy(src, dst, sem).start()

            @pl.when(jnp.logical_not(own))
            def _():
                rcopy(src, dst, e_s.at[i], sem, to).start()

    e_start(0)

    def b_parts(i, out):
        xs, g2 = lax.rem(x + 7 - lax.div(i, 2) + zl, 4), lax.rem(i, 2)
        own = (g2 == g) & (xs == zl) & (x1 == x) & (c1 == c)
        dst = out.at[pl.ds(pl.multiple_of(zl * 512, 512), 512), :]
        return own, abuf.at[xs], dst, dev(g2, xs, y, x1, c1)

    def b_step(m):
        xs = lax.rem(x + 7 - m + zl, 4)
        arrived(abuf.at[xs], a_r.at[xs])
        for w, out in ((0, gate_out), (1, up_out)):

            @pl.when(c == w)
            def _():
                @pl.loop(2 * m, 2 * m + 2)
                def _(i):
                    own, src, dst, to = b_parts(i, out)

                    @pl.when(own)
                    def _():
                        pltpu.make_async_copy(src, dst, b_r.at[w, zl]).start()

                    @pl.when(jnp.logical_not(own))
                    def _():
                        rcopy(src, dst, b_s.at[i], b_r.at[w, zl], to).start()

    def nth(j):
        return lax.rem(zl + 4 + j * (1 - 2 * lax.div(zl, 2)), 4)

    for m in range(4):
        b_step(m)
        if m < 3:
            q = nth(m + 1)
            arrived(rows.at[y, q], t_r.at[q])
            r_send(1, q).start()
            l_send(1, q).start()

    e_start(4)

    def ring_step(s):
        @pl.loop(0, 4)
        def _(j):
            q = nth(j)
            arrived(rows.at[lax.rem(y - s + 9, 8), q], y_r.at[0, s - 1, q])
            arrived(rows.at[lax.rem(y + s + 7, 8), q], y_r.at[1, s - 1, q])
            if s < 4:
                r_send(s, q).start()
                l_send(s, q).start()
            else:

                @pl.when(q < 2)
                def _():
                    r_send(s, q).start()

                @pl.when(q >= 2)
                def _():
                    l_send(s, q).start()

    for s in (2, 3, 4):
        ring_step(s)

    far = lax.rem(y + 4, 8)
    for q in range(4):
        arrived(rows.at[far, q], y_r.at[q // 2, 4, q])
    for m in range(4):
        q = lax.rem(zl + m - xe + 5, 4)
        at = pl.ds(pl.multiple_of(q * 512, 512), 512)
        arrived(gate_out.at[at, :], b_r.at[0, q])
        arrived(up_out.at[at, :], b_r.at[1, q])

        @pl.loop(0, 4)
        def _(i):
            x_in = rows[pl.ds(2 * i, 2), :, :, at].reshape(8 * SLOTS, 512)
            gate_part = jnp.dot(x_in, gate_out[at, :], preferred_element_type=F32)
            up_part = jnp.dot(x_in, up_out[at, :], preferred_element_type=F32)
            if m > 0:
                gate_part = gate_part + acc[0, i]
                up_part = up_part + acc[1, i]
            if m < 3:
                acc[0, i] = gate_part
                acc[1, i] = up_part
            else:
                hid[i] = (gate_part / (1.0 + jnp.exp(-gate_part)) * up_part).astype(BF)

    def target(way, s):
        return lax.rem(y + 5 - s, 8) if way == 0 else lax.rem(y + 3 + s, 8)

    def send(way, s, q, src):
        return rcopy(
            src, got.at[way, s - 1, q], p_s.at[way, s - 1, q], p_r.at[way, s - 1, q], (right, left)[way]
        )

    def first_hand(way, s, q):
        return s == 1 or (s == 2 and q // 2 != way)

    def source(way, s, q):
        if first_hand(way, s, q):
            return part.at[target(way, s), q]
        return keep.at[way, s - 2, q]

    def make(q):
        for h in range(2):
            at = down_out.at[h * 128 : (h + 1) * 128, q * 512 : (q + 1) * 512]
            arrived(at, e_r.at[h, q])

        @pl.loop(0, 4)
        def _(i):
            made = jnp.dot(
                hid[i], down_out[:, q * 512 : (q + 1) * 512], preferred_element_type=F32
            ).astype(BF)
            part[2 * i, q] = made[:128]
            part[2 * i + 1, q] = made[128:]

        send(q // 2, 1, q, source(q // 2, 1, q)).start()
        send(1 - q // 2, 2, q, source(1 - q // 2, 2, q)).start()

    def pass_on(way, s, q):
        arrived(got.at[way, s - 2, q], p_r.at[way, s - 2, q])
        total = part[target(way, s), q].astype(F32) + got[way, s - 2, q].astype(F32)
        keep[way, s - 2, q] = total.astype(BF)
        send(way, s, q, source(way, s, q)).start()

    for q in (0, 1, 2, 3):
        make(q)
    for s, order in ((2, (0, 1)), (3, (2, 3, 0, 1)), (4, (2, 0, 3, 1))):
        for j in order:
            for way in range(2):
                pass_on(way, s, (j + 2 * way) % 4)

    def f_send(q, j):
        to = lax.rem(zl + j, 4)
        src = fin.at[q, pl.ds(pl.multiple_of(to * 32, 32), 32), :]
        return rcopy(src, gotz.at[q, zl], z_s.at[q], z_r.at[q], dev(g, to, y, x, c))

    def finish(q):
        for way in range(2):
            arrived(got.at[way, 3, q], p_r.at[way, 3, q])
        total = part[y, q].astype(F32) + got[0, 3, q].astype(F32) + got[1, 3, q].astype(F32)
        fin[q] = total.astype(BF)

        @pl.loop(1, 4)
        def _(j):
            f_send(q, j).start()

    def c_send(q, j):
        t = lax.rem(me_t + j, 8)
        return rcopy(
            sendc.at[q, t], gotc.at[q, me_t], c_s.at[q], c_r.at[q], (g, zl * 8 + y, t)
        )

    def spread(q):
        out = fin[q, pl.ds(pl.multiple_of(zl * 32, 32), 32), :].astype(F32)
        arrived(gotz.at[q, 0:3], z_r.at[q])
        for j in range(1, 4):
            out = out + gotz[q, lax.rem(zl + j, 4)].astype(F32)
        term = (out * wslot).astype(BF)
        wide = lax.dot_general(
            chosen, term, (((0,), (0,)), ((), ())), preferred_element_type=F32
        ).astype(BF)
        for t in range(8):
            sendc[q, t] = wide[t * 16 : (t + 1) * 16, :]

        @pl.loop(1, 8)
        def _(j):
            c_send(q, j).start()

    def settle(q):
        arrived(gotc.at[q, 0:7], c_r.at[q])
        total = sendc[q, me_t].astype(F32)
        for j in range(1, 8):
            total = total + gotc[q, lax.rem(me_t + j, 8)].astype(F32)
        mixed[:, q * 512 : (q + 1) * 512] = total.astype(BF)

    @pl.loop(1, 4)
    def _(j):
        z_send(j).wait_send()

    @pl.loop(0, 8)
    def _(i):
        own, src, dst, to = d_parts(i)

        @pl.when(jnp.logical_not(own))
        def _():
            rcopy(src, dst, d_s.at[i], d_r.at[x], to).wait_send()

    @pl.loop(0, 32)
    def _(i):
        own, src, dst, to = a_parts(i)

        @pl.when(jnp.logical_not(own))
        def _():
            rcopy(src, dst, a_s.at[i], a_r.at[x], to).wait_send()

    @pl.loop(0, 8)
    def _(i):
        own, src, dst, to, sem = e_parts(i)

        @pl.when(jnp.logical_not(own))
        def _():
            rcopy(src, dst, e_s.at[i], sem, to).wait_send()

    @pl.loop(0, 8)
    def _(i):
        own, src, dst, to = b_parts(i, gate_out)

        @pl.when(jnp.logical_not(own))
        def _():
            rcopy(src, dst, b_s.at[i], b_r.at[0, zl], to).wait_send()

    for s in (1, 2, 3):

        @pl.loop(0, 4)
        def _(q):
            r_send(s, q).wait_send()
            l_send(s, q).wait_send()

    for q in range(2):
        r_send(4, q).wait_send()
        l_send(4, q + 2).wait_send()

    for s in (1, 2, 3):
        for q in range(4):
            for way in range(2):
                if s > 1 or q // 2 == way:
                    send(way, s, q, source(way, s, q)).wait_send()

    for q in (0, 2, 1, 3):
        finish(q)
    for q in (0, 2, 1, 3):
        spread(q)
    for q in range(4):
        for way in range(2):
            send(way, 4, q, source(way, 4, q)).wait_send()
        arrived(fin.at[q, 0:96, :], z_s.at[q])
    for q in (0, 2, 1, 3):
        settle(q)
    for q in range(4):
        arrived(sendc.at[q, 0:7], c_s.at[q])


VM = pl.BlockSpec(memory_space=pltpu.VMEM)
HB = pl.BlockSpec(memory_space=pltpu.MemorySpace.HBM)
DMA = pltpu.SemaphoreType.DMA


def store_kernel(*refs):
    copies = [pltpu.make_async_copy(refs[i], refs[4 + i], refs[8].at[i]) for i in range(4)]
    for one in copies:
        one.start()
    for one in copies:
        one.wait()


def body(prompt, expert_ids, route_weights, gate_master, up_master, down_master, ffn_gain):
    made = pl.pallas_call(
        kernel,
        out_shape=(
            jax.ShapeDtypeStruct((D, 256), BF),
            jax.ShapeDtypeStruct((D, 256), BF),
            jax.ShapeDtypeStruct((256, D), BF),
            jax.ShapeDtypeStruct((16, D), BF),
        ),
        in_specs=[HB] * 4 + [VM] * 3,
        out_specs=(VM,) * 4,
        scratch_shapes=[
            pltpu.VMEM((TOK, D), BF),
            pltpu.VMEM((4, 64, 1024), F32),
            pltpu.VMEM((4, 64, 1024), F32),
            pltpu.VMEM((4, 256, 256), F32),
            pltpu.VMEM((2, 4, 4, 64, 256), BF),
            pltpu.VMEM((4, 2, 128, 256), BF),
            pltpu.VMEM((4, 512, 256), BF),
            pltpu.VMEM((4, 128, 512), BF),
            pltpu.VMEM((8, 4, SLOTS, D), BF),
            pltpu.VMEM((2, 4, 256, 256), F32),
            pltpu.VMEM((4, 256, 256), BF),
            pltpu.VMEM((8, 4, 128, 512), BF),
            pltpu.VMEM((2, 3, 4, 128, 512), BF),
            pltpu.VMEM((2, 4, 4, 128, 512), BF),
            pltpu.VMEM((4, 128, 512), BF),
            pltpu.VMEM((4, 4, SLOTS, 512), BF),
            pltpu.VMEM((4, 8, 16, 512), BF),
            pltpu.VMEM((4, 8, 16, 512), BF),
            DMA((4,)),
            DMA((32,)),
            DMA((4,)),
            DMA((8,)),
            DMA((4,)),
            DMA((8,)),
            DMA((2, 4)),
            DMA((8,)),
            DMA((2, 4)),
            DMA((4,)),
            DMA((4,)),
            DMA((2, 5, 4)),
            DMA((2, 5, 4)),
            DMA((2, 4, 4)),
            DMA((2, 4, 4)),
            DMA((4,)),
            DMA((4,)),
            DMA((4,)),
            DMA((4,)),
        ],
        compiler_params=pltpu.CompilerParams(
            collective_id=0, has_side_effects=True, vmem_limit_bytes=36 << 20
        ),
        name="serve",
    )(
        *(
            pltpu.with_memory_space_constraint(v, pltpu.MemorySpace.HBM)
            for v in (prompt, gate_master, up_master, down_master)
        ),
        expert_ids.T, route_weights.T, ffn_gain[None],
    )
    gate, up, down, mixed = pl.pallas_call(
        store_kernel,
        out_shape=tuple(jax.ShapeDtypeStruct(v.shape, BF) for v in made),
        in_specs=[VM] * 4,
        out_specs=(HB,) * 4,
        scratch_shapes=[DMA((4,))],
        compiler_params=pltpu.CompilerParams(vmem_limit_bytes=8 << 20),
        name="store",
    )(*made)
    return gate[None], up[None], down[None], mixed


def solution(mesh):
    return jax.shard_map(
        body,
        mesh=mesh,
        in_specs=(
            P(("gr", "fs"), None),
            P(("gr", "fs"), None),
            P(("gr", "fs"), None),
            P("gr", "fs", "tp"),
            P("gr", "fs", "tp"),
            P("gr", "fs", "tp"),
            P("fs"),
        ),
        out_specs=(
            P("tp", None, "fs"),
            P("tp", None, "fs"),
            P("tp", "fs", None),
            P(("gr", "fs", "tp"), None),
        ),
        check_vma=False,
    )
```

```python
import jax
import jax.numpy as jnp
from jax import lax
from jax.experimental import pallas as pl
from jax.experimental.pallas import tpu as pltpu
from jax.sharding import PartitionSpec as P

EXPERTS = 8
SLOTS = 32
TOK = 128
D = 2048
NORM_EPS = 1e-06
MESH = pl.DeviceIdType.MESH
BF = jnp.bfloat16
F32 = jnp.float32


def place():
    g, f, t = lax.axis_index("gr"), lax.axis_index("fs"), lax.axis_index("tp")
    return g, lax.div(f, 8), lax.rem(f, 8), lax.div(t, 2), lax.rem(t, 2)


def dev(g, zl, y, x, c):
    return (g, zl * 8 + y, x * 2 + c)


def signal(sem, where):
    pl.semaphore_signal(sem, inc=1, device_id=where, device_id_type=MESH)


def rcopy(src, dst, ssem, rsem, where):
    return pltpu.make_async_remote_copy(
        src_ref=src, dst_ref=dst, send_sem=ssem, recv_sem=rsem, device_id=where, device_id_type=MESH
    )


def arrived(buf, sem):
    pltpu.make_async_copy(buf, buf, sem).wait()


def home_of(g, el):
    odd = lax.rem(el, 2)
    x1 = 2 * g + lax.div(el, 2)
    return x1, odd, x1 * (1 - odd) + (3 - x1) * odd


def served_by(g, x):
    h = lax.div(x, 2)
    c1 = h + g - 2 * h * g
    return x * (1 - c1) + (3 - x) * c1, c1


def choice_matrix(ids):
    e = lax.axis_index("tp")
    mine = jnp.sum((ids == e).astype(F32), axis=0, keepdims=True)
    mine = jnp.broadcast_to(mine, (SLOTS, TOK))
    row = lax.broadcasted_iota(jnp.int32, (TOK, TOK), 0)
    col = lax.broadcasted_iota(jnp.int32, (TOK, TOK), 1)
    before = (row < col).astype(BF)
    rank = jnp.dot(mine.astype(BF), before, preferred_element_type=F32)
    slot = lax.broadcasted_iota(jnp.int32, (SLOTS, TOK), 0).astype(F32)
    return jnp.where((mine > 0.5) & (jnp.abs(rank - slot) < 0.5), 1.0, 0.0)


def kernel(
    prompt_h, gate_h, up_h, down_h, ids, weights, gain,
    gate_out, up_out, down_out, mixed,
    prompt, gate, up, down, stg, stgd, abuf, dbuf, rows,
    acc, hid, part, keep, got, fin, gotz, sendc, gotc,
    in_s, a_s, a_r, d_s, d_r, b_s, b_r, e_s, e_r, t_s, t_r, y_s, y_r,
    p_s, p_r, z_s, z_r, c_s, c_r,
):
    loads = [
        pltpu.make_async_copy(src, dst, in_s.at[i])
        for i, (src, dst) in enumerate(
            ((prompt_h, prompt), (down_h, down), (gate_h, gate), (up_h, up))
        )
    ]
    for load in loads:
        load.start()
    g, zl, y, x, c = place()
    me_t = x * 2 + c
    barrier = pltpu.get_barrier_semaphore()
    right = dev(g, zl, lax.rem(y + 1, 8), x, c)
    left = dev(g, zl, lax.rem(y + 7, 8), x, c)
    half = lax.div(y, 4)
    x1, c1 = served_by(g, x)
    ge = lax.div(x, 2)
    _, _, xe = home_of(ge, lax.rem(me_t, 4))

    @pl.loop(0, 32)
    def _(i):
        xs, ys = lax.div(i, 8), lax.rem(i, 8)

        @pl.when((xs != x) | (ys != y) | (half != c))
        def _():
            signal(barrier, dev(g, zl, ys, xs, half))

    @pl.loop(0, 8)
    def _(i):
        @pl.when(i != me_t)
        def _():
            signal(barrier, (g, zl * 8 + y, i))

        zs, w = lax.div(i, 2), lax.rem(i, 2)

        @pl.when((ge != g) | (zs != zl) | (xe != x) | (w != c))
        def _():
            signal(barrier, dev(ge, zs, y, xe, w))

    @pl.loop(1, 4)
    def _(j):
        signal(barrier, dev(g, lax.rem(zl + j, 4), y, x, c))

    signal(barrier, right)
    signal(barrier, left)

    choice = choice_matrix(ids[...])
    wslot = jnp.sum(
        choice
        * jnp.sum(jnp.where(ids[...] == me_t, weights[...], 0.0), axis=0, keepdims=True),
        axis=1,
        keepdims=True,
    )
    chosen = choice.astype(BF)
    loads[0].wait()
    xf = prompt[...].astype(F32)
    normed = (xf * lax.rsqrt(jnp.mean(xf * xf, axis=1, keepdims=True) + NORM_EPS)).astype(BF)
    rows[y, zl] = jnp.dot(chosen, normed, preferred_element_type=F32).astype(BF)

    loads[1].wait()

    @pl.loop(0, 4)
    def _(el):
        for h in range(2):
            stgd[el, h] = down[el, h * 128 : (h + 1) * 128, :].astype(BF)

    eye = lax.broadcasted_iota(jnp.int32, (64, 64), 0) == lax.broadcasted_iota(jnp.int32, (64, 64), 1)
    col = jnp.sum(
        jnp.where(eye, jnp.broadcast_to(gain[...], (64, 64)), 0.0), axis=1, keepdims=True
    )
    loads[2].wait()
    loads[3].wait()

    @pl.loop(0, 4)
    def _(el):
        for k in range(4):
            cols = slice(k * 256, (k + 1) * 256)
            stg[0, el, k] = (gate[el, :, cols] * col).astype(BF)
            stg[1, el, k] = (up[el, :, cols] * col).astype(BF)

    same_half = jnp.where(half == c, 1, 0)
    own_b = jnp.where(ge == g, 1, 0) * (1 - c)
    pl.semaphore_wait(barrier, 32 - same_half + 7 + 8 - own_b + 3 + 2)

    def z_send(j):
        to = lax.rem(zl + j, 4)
        return rcopy(rows.at[y, zl], rows.at[y, zl], t_s.at[j], t_r.at[zl], dev(g, to, y, x, c))

    def r_send(s, q):
        at = lax.rem(y - s + 9, 8)
        return rcopy(rows.at[at, q], rows.at[at, q], y_s.at[0, s, q], y_r.at[0, s, q], right)

    def l_send(s, q):
        at = lax.rem(y + s + 7, 8)
        return rcopy(rows.at[at, q], rows.at[at, q], y_s.at[1, s, q], y_r.at[1, s, q], left)

    @pl.loop(1, 4)
    def _(j):
        z_send(j).start()

    def collected(x2):
        x0, c0 = served_by(g, x2)
        return 2 * (x0 - 2 * g) + c0

    def d_parts(i):
        x2, h = lax.rem(x + 1 + lax.div(i, 2), 4), lax.rem(i, 2)
        own = (x2 == x) & (h == c)
        dst = dbuf.at[x, :, pl.ds(pl.multiple_of(c * 256, 256), 256)]
        return own, stgd.at[collected(x2), h], dst, dev(g, zl, y, x2, h)

    @pl.loop(0, 8)
    def _(i):
        own, src, dst, to = d_parts(i)

        @pl.when(own)
        def _():
            pltpu.make_async_copy(src, dst, d_r.at[x]).start()

        @pl.when(jnp.logical_not(own))
        def _():
            rcopy(src, dst, d_s.at[i], d_r.at[x], to).start()

    r_send(1, zl).start()
    l_send(1, zl).start()

    def a_parts(i):
        k, w = lax.rem(y + lax.rem(lax.div(i, 2), 4), 4), lax.rem(i, 2)
        x2 = lax.rem(x + 5 + lax.div(i, 8) - zl, 4)
        el, y2 = collected(x2), 4 * c + k
        own = (x2 == x) & (w == c) & (y2 == y)
        dst = abuf.at[x, pl.ds(pl.multiple_of(y * 64, 64), 64), :]
        return own, stg.at[w, el, k], dst, dev(g, zl, y2, x2, w)

    @pl.loop(0, 32)
    def _(i):
        own, src, dst, to = a_parts(i)

        @pl.when(own)
        def _():
            pltpu.make_async_copy(src, dst, a_r.at[x]).start()

        @pl.when(jnp.logical_not(own))
        def _():
            rcopy(src, dst, a_s.at[i], a_r.at[x], to).start()

    def e_parts(i):
        j, g2 = lax.div(i, 2), lax.rem(i, 2)
        own = (g2 == g) & (x1 == x) & (c1 == c)
        dst = down_out.at[
            pl.ds(pl.multiple_of(c * 128, 128), 128), pl.ds(pl.multiple_of(j * 512, 512), 512)
        ]
        return own, dbuf.at[j], dst, dev(g2, zl, y, x1, c1), e_r.at[c, j]

    def e_start(first):
        @pl.loop(first, first + 4)
        def _(i):
            own, src, dst, to, sem = e_parts(i)

            @pl.when(lax.rem(i, 2) == 0)
            def _():
                arrived(src, d_r.at[lax.div(i, 2)])

            @pl.when(own)
            def _():
                pltpu.make_async_copy(src, dst, sem).start()

            @pl.when(jnp.logical_not(own))
            def _():
                rcopy(src, dst, e_s.at[i], sem, to).start()

    e_start(0)

    def b_parts(i, out):
        xs, g2 = lax.rem(x + 7 - lax.div(i, 2) + zl, 4), lax.rem(i, 2)
        own = (g2 == g) & (xs == zl) & (x1 == x) & (c1 == c)
        dst = out.at[pl.ds(pl.multiple_of(zl * 512, 512), 512), :]
        return own, abuf.at[xs], dst, dev(g2, xs, y, x1, c1)

    def b_step(m):
        xs = lax.rem(x + 7 - m + zl, 4)
        arrived(abuf.at[xs], a_r.at[xs])
        for w, out in ((0, gate_out), (1, up_out)):

            @pl.when(c == w)
            def _():
                @pl.loop(2 * m, 2 * m + 2)
                def _(i):
                    own, src, dst, to = b_parts(i, out)

                    @pl.when(own)
                    def _():
                        pltpu.make_async_copy(src, dst, b_r.at[w, zl]).start()

                    @pl.when(jnp.logical_not(own))
                    def _():
                        rcopy(src, dst, b_s.at[i], b_r.at[w, zl], to).start()

    def nth(j):
        return lax.rem(zl + 4 + j * (1 - 2 * lax.div(zl, 2)), 4)

    for m in range(4):
        b_step(m)
        if m < 3:
            q = nth(m + 1)
            arrived(rows.at[y, q], t_r.at[q])
            r_send(1, q).start()
            l_send(1, q).start()

    e_start(4)

    def ring_step(s):
        @pl.loop(0, 4)
        def _(j):
            q = nth(j)
            arrived(rows.at[lax.rem(y - s + 9, 8), q], y_r.at[0, s - 1, q])
            arrived(rows.at[lax.rem(y + s + 7, 8), q], y_r.at[1, s - 1, q])
            if s < 4:
                r_send(s, q).start()
                l_send(s, q).start()
            else:

                @pl.when(q < 2)
                def _():
                    r_send(s, q).start()

                @pl.when(q >= 2)
                def _():
                    l_send(s, q).start()

    for s in (2, 3, 4):
        ring_step(s)

    far = lax.rem(y + 4, 8)
    for q in range(4):
        arrived(rows.at[far, q], y_r.at[q // 2, 4, q])
    for m in range(4):
        q = lax.rem(zl + m - xe + 5, 4)
        at = pl.ds(pl.multiple_of(q * 512, 512), 512)
        arrived(gate_out.at[at, :], b_r.at[0, q])
        arrived(up_out.at[at, :], b_r.at[1, q])

        @pl.loop(0, 4)
        def _(i):
            x_in = rows[pl.ds(2 * i, 2), :, :, at].reshape(8 * SLOTS, 512)
            gate_part = jnp.dot(x_in, gate_out[at, :], preferred_element_type=F32)
            up_part = jnp.dot(x_in, up_out[at, :], preferred_element_type=F32)
            if m > 0:
                gate_part = gate_part + acc[0, i]
                up_part = up_part + acc[1, i]
            if m < 3:
                acc[0, i] = gate_part
                acc[1, i] = up_part
            else:
                hid[i] = (gate_part / (1.0 + jnp.exp(-gate_part)) * up_part).astype(BF)

    def target(way, s):
        return lax.rem(y + 5 - s, 8) if way == 0 else lax.rem(y + 3 + s, 8)

    def send(way, s, q, src):
        return rcopy(
            src, got.at[way, s - 1, q], p_s.at[way, s - 1, q], p_r.at[way, s - 1, q], (right, left)[way]
        )

    def first_hand(way, s, q):
        return s == 1 or (s == 2 and q // 2 != way)

    def source(way, s, q):
        if first_hand(way, s, q):
            return part.at[target(way, s), q]
        return keep.at[way, s - 2, q]

    def make(q):
        for h in range(2):
            at = down_out.at[h * 128 : (h + 1) * 128, q * 512 : (q + 1) * 512]
            arrived(at, e_r.at[h, q])

        @pl.loop(0, 4)
        def _(i):
            made = jnp.dot(
                hid[i], down_out[:, q * 512 : (q + 1) * 512], preferred_element_type=F32
            ).astype(BF)
            part[2 * i, q] = made[:128]
            part[2 * i + 1, q] = made[128:]

        send(q // 2, 1, q, source(q // 2, 1, q)).start()
        send(1 - q // 2, 2, q, source(1 - q // 2, 2, q)).start()

    def pass_on(way, s, q):
        arrived(got.at[way, s - 2, q], p_r.at[way, s - 2, q])
        total = part[target(way, s), q].astype(F32) + got[way, s - 2, q].astype(F32)
        keep[way, s - 2, q] = total.astype(BF)
        send(way, s, q, source(way, s, q)).start()

    for q in (0, 1, 2, 3):
        make(q)
    for s, order in ((2, (0, 1)), (3, (2, 3, 0, 1)), (4, (2, 0, 3, 1))):
        for j in order:
            for way in range(2):
                pass_on(way, s, (j + 2 * way) % 4)

    def f_send(q, to):
        src = fin.at[q, pl.ds(pl.multiple_of(to * 32, 32), 32), :]
        return rcopy(src, gotz.at[q, zl], z_s.at[q], z_r.at[q], dev(g, to, y, x, c))

    def finish(q):
        for way in range(2):
            arrived(got.at[way, 3, q], p_r.at[way, 3, q])
        total = part[y, q].astype(F32) + got[0, 3, q].astype(F32) + got[1, 3, q].astype(F32)
        fin[q] = total.astype(BF)

        @pl.loop(0, 4)
        def _(to):
            @pl.when(to != zl)
            def _():
                f_send(q, to).start()

    def c_send(q, j):
        t = lax.rem(me_t + j, 8)
        return rcopy(
            sendc.at[q, t], gotc.at[q, me_t], c_s.at[q], c_r.at[q], (g, zl * 8 + y, t)
        )

    def spread(q):
        out = fin[q, pl.ds(pl.multiple_of(zl * 32, 32), 32), :].astype(F32)
        arrived(gotz.at[q, 0:3], z_r.at[q])
        for j in range(1, 4):
            out = out + gotz[q, lax.rem(zl + j, 4)].astype(F32)
        term = (out * wslot).astype(BF)
        wide = lax.dot_general(
            chosen, term, (((0,), (0,)), ((), ())), preferred_element_type=F32
        ).astype(BF)
        for t in range(8):
            sendc[q, t] = wide[t * 16 : (t + 1) * 16, :]

        @pl.loop(1, 8)
        def _(j):
            c_send(q, j).start()

    def settle(q):
        arrived(gotc.at[q, 0:7], c_r.at[q])
        total = sendc[q, me_t].astype(F32)
        for j in range(1, 8):
            total = total + gotc[q, lax.rem(me_t + j, 8)].astype(F32)
        mixed[:, q * 512 : (q + 1) * 512] = total.astype(BF)

    @pl.loop(1, 4)
    def _(j):
        z_send(j).wait_send()

    @pl.loop(0, 8)
    def _(i):
        own, src, dst, to = d_parts(i)

        @pl.when(jnp.logical_not(own))
        def _():
            rcopy(src, dst, d_s.at[i], d_r.at[x], to).wait_send()

    @pl.loop(0, 32)
    def _(i):
        own, src, dst, to = a_parts(i)

        @pl.when(jnp.logical_not(own))
        def _():
            rcopy(src, dst, a_s.at[i], a_r.at[x], to).wait_send()

    @pl.loop(0, 8)
    def _(i):
        own, src, dst, to, sem = e_parts(i)

        @pl.when(jnp.logical_not(own))
        def _():
            rcopy(src, dst, e_s.at[i], sem, to).wait_send()

    @pl.loop(0, 8)
    def _(i):
        own, src, dst, to = b_parts(i, gate_out)

        @pl.when(jnp.logical_not(own))
        def _():
            rcopy(src, dst, b_s.at[i], b_r.at[0, zl], to).wait_send()

    for s in (1, 2, 3):

        @pl.loop(0, 4)
        def _(q):
            r_send(s, q).wait_send()
            l_send(s, q).wait_send()

    for q in range(2):
        r_send(4, q).wait_send()
        l_send(4, q + 2).wait_send()

    for s in (1, 2, 3):
        for q in range(4):
            for way in range(2):
                if s > 1 or q // 2 == way:
                    send(way, s, q, source(way, s, q)).wait_send()

    for q in (0, 2, 1, 3):
        finish(q)
    for q in (0, 2, 1, 3):
        spread(q)
    for q in range(4):
        for way in range(2):
            send(way, 4, q, source(way, 4, q)).wait_send()
        arrived(fin.at[q, 0:96, :], z_s.at[q])
    for q in (0, 2, 1, 3):
        settle(q)
    for q in range(4):
        arrived(sendc.at[q, 0:7], c_s.at[q])


VM = pl.BlockSpec(memory_space=pltpu.VMEM)
HB = pl.BlockSpec(memory_space=pltpu.MemorySpace.HBM)
DMA = pltpu.SemaphoreType.DMA


def store_kernel(*refs):
    copies = [pltpu.make_async_copy(refs[i], refs[4 + i], refs[8].at[i]) for i in range(4)]
    for one in copies:
        one.start()
    for one in copies:
        one.wait()


def body(prompt, expert_ids, route_weights, gate_master, up_master, down_master, ffn_gain):
    made = pl.pallas_call(
        kernel,
        out_shape=(
            jax.ShapeDtypeStruct((D, 256), BF),
            jax.ShapeDtypeStruct((D, 256), BF),
            jax.ShapeDtypeStruct((256, D), BF),
            jax.ShapeDtypeStruct((16, D), BF),
        ),
        in_specs=[HB] * 4 + [VM] * 3,
        out_specs=(VM,) * 4,
        scratch_shapes=[
            pltpu.VMEM((TOK, D), BF),
            pltpu.VMEM((4, 64, 1024), F32),
            pltpu.VMEM((4, 64, 1024), F32),
            pltpu.VMEM((4, 256, 256), F32),
            pltpu.VMEM((2, 4, 4, 64, 256), BF),
            pltpu.VMEM((4, 2, 128, 256), BF),
            pltpu.VMEM((4, 512, 256), BF),
            pltpu.VMEM((4, 128, 512), BF),
            pltpu.VMEM((8, 4, SLOTS, D), BF),
            pltpu.VMEM((2, 4, 256, 256), F32),
            pltpu.VMEM((4, 256, 256), BF),
            pltpu.VMEM((8, 4, 128, 512), BF),
            pltpu.VMEM((2, 3, 4, 128, 512), BF),
            pltpu.VMEM((2, 4, 4, 128, 512), BF),
            pltpu.VMEM((4, 128, 512), BF),
            pltpu.VMEM((4, 4, SLOTS, 512), BF),
            pltpu.VMEM((4, 8, 16, 512), BF),
            pltpu.VMEM((4, 8, 16, 512), BF),
            DMA((4,)),
            DMA((32,)),
            DMA((4,)),
            DMA((8,)),
            DMA((4,)),
            DMA((8,)),
            DMA((2, 4)),
            DMA((8,)),
            DMA((2, 4)),
            DMA((4,)),
            DMA((4,)),
            DMA((2, 5, 4)),
            DMA((2, 5, 4)),
            DMA((2, 4, 4)),
            DMA((2, 4, 4)),
            DMA((4,)),
            DMA((4,)),
            DMA((4,)),
            DMA((4,)),
        ],
        compiler_params=pltpu.CompilerParams(
            collective_id=0, has_side_effects=True, vmem_limit_bytes=36 << 20
        ),
        name="serve",
    )(
        *(
            pltpu.with_memory_space_constraint(v, pltpu.MemorySpace.HBM)
            for v in (prompt, gate_master, up_master, down_master)
        ),
        expert_ids.T, route_weights.T, ffn_gain[None],
    )
    gate, up, down, mixed = pl.pallas_call(
        store_kernel,
        out_shape=tuple(jax.ShapeDtypeStruct(v.shape, BF) for v in made),
        in_specs=[VM] * 4,
        out_specs=(HB,) * 4,
        scratch_shapes=[DMA((4,))],
        compiler_params=pltpu.CompilerParams(vmem_limit_bytes=8 << 20),
        name="store",
    )(*made)
    return gate[None], up[None], down[None], mixed


def solution(mesh):
    return jax.shard_map(
        body,
        mesh=mesh,
        in_specs=(
            P(("gr", "fs"), None),
            P(("gr", "fs"), None),
            P(("gr", "fs"), None),
            P("gr", "fs", "tp"),
            P("gr", "fs", "tp"),
            P("gr", "fs", "tp"),
            P("fs"),
        ),
        out_specs=(
            P("tp", None, "fs"),
            P("tp", None, "fs"),
            P("tp", "fs", None),
            P(("gr", "fs", "tp"), None),
        ),
        check_vma=False,
    )
```
